512 devices in a mesh: grp: 2 (over y), fs: 32 (over z), tp: 8 (over x, core).
Axes of the slice: x: 4, y: 2, z: 32, core: 2. Of those that a mesh axis runs over, the one named last changes fastest.
The devices are a block of a 4x8x32 slice.
Arguments:
- stream: bfloat16 [2048, 24576], P('tp', ('grp', 'fs')), parts along dimension 1, may hold values from -6 to 6
- mixer_gain: float32 [2048], replicated, may hold values from 0.1 to 1.9
- glu_value: bfloat16 [2048, 1024], P('fs', 'tp'), may hold values from -0.125 to 0.125
- glu_gate: bfloat16 [2048, 1024], P('fs', 'tp'), may hold values from -0.125 to 0.125
- conv_kernel: bfloat16 [31, 1024], replicated, may hold values from -1 to 1
- channel_gain: float32 [1024], replicated, may hold values from 0.1 to 1.9
- conv_out: bfloat16 [2048, 1024], P('fs', 'tp'), may hold values from -0.1875 to 0.1875
- ffn_gain: float32 [2048], replicated, may hold values from 0.1 to 1.9
- ffn_gate: bfloat16 [2048, 5632], P('fs', 'tp'), may hold values from -0.125 to 0.125
- ffn_up: bfloat16 [2048, 5632], P('fs', 'tp'), may hold values from -0.125 to 0.125
- ffn_down: bfloat16 [2048, 5632], P('fs', 'tp'), may hold values from -0.078125 to 0.078125
Outputs:
- result: bfloat16 [2048, 24576], P('tp', ('grp', 'fs')), parts along dimension 1
The draws below stay inside these ranges and needn't reach their ends.
There are 2 independent parts, one for each index of `grp`. The reference program is written for one: setup_inputs(seed, part) draws one part's arguments, and reference() takes and returns one part's arrays. A program takes and returns all parts, laid end to end along the dimension named above; an argument that names none is the same for every part. Nothing has to cross between parts.
All inputs are finite; a program needn't handle non-finite values.
Results may differ from the reference program's by a relative error of at most 0.018.
Values may be sent and summed in bfloat16 or wider, within the bound.
A program may use at most 64 MiB of HBM per device.

```python
import jax
import jax.numpy as jnp
from jax import lax

D = 2048
DC = 1024
FF = 5632
KERNEL = 31
TOK_DEV = 384
TOKENS = 12288
N_TP = 8


def steps_of(stream_key, shape, pieces, low, largest):
    level, own = 1.0, jax.random.fold_in(stream_key, 6)
    for dim, blocks in pieces:
        steps = jnp.exp(jax.random.uniform(jax.random.fold_in(own, dim), (blocks,), jnp.float32, low / len(pieces), largest / len(pieces)))
        level = level * jnp.repeat(steps, shape[dim] // blocks).reshape([-1 if axis == dim else 1 for axis in range(len(shape))])
    return level


def bell_draw(rng, shape, deviation, limit, pieces=(), kind=jnp.bfloat16):
    entries = jax.random.normal(rng, shape, jnp.float32) * deviation
    if len(pieces) > 0:
        entries = steps_of(rng, shape, pieces, -0.22, 0.18) * entries
    return jnp.clip(entries, min=-limit, max=limit).astype(kind)


def setup_inputs(seed: int = 0, part: int = 0) -> dict:
    splits = jax.random.split(jax.random.key(seed), 12)
    part_keys = jax.random.split(jax.random.fold_in(splits[11], part), 12)
    return {
        "stream": bell_draw(part_keys[0], (D, TOKENS), 1.0, 6.0, ((0, 8), (1, 32))),
        "mixer_gain": jnp.clip(1.0 + 0.18 * jax.random.normal(splits[1], (D,), jnp.float32), 0.1, 1.9),
        "glu_value": bell_draw(splits[2], (D, DC), D ** -0.5, 0.125, ((0, 32), (1, 8))),
        "glu_gate": bell_draw(splits[3], (D, DC), D ** -0.5, 0.125, ((0, 32), (1, 8))),
        "conv_kernel": bell_draw(splits[4], (KERNEL, DC), KERNEL ** -0.5, 1.0),
        "channel_gain": jnp.clip(1.0 + 0.18 * jax.random.normal(splits[5], (DC,), jnp.float32), 0.1, 1.9),
        "conv_out": bell_draw(splits[6], (D, DC), DC ** -0.5, 0.1875, ((0, 32), (1, 8))),
        "ffn_gain": jnp.clip(1.0 + 0.18 * jax.random.normal(splits[7], (D,), jnp.float32), 0.1, 1.9),
        "ffn_gate": bell_draw(splits[8], (D, FF), D ** -0.5, 0.125, ((0, 32), (1, 8))),
        "ffn_up": bell_draw(splits[9], (D, FF), D ** -0.5, 0.125, ((0, 32), (1, 8))),
        "ffn_down": bell_draw(splits[10], (D, FF), FF ** -0.5, 0.078125, ((0, 32), (1, 8))),
    }


def rms_normalize(wide, gain):
    inverse = lax.rsqrt(lax.optimization_barrier(jnp.mean(wide * wide, axis=0, keepdims=True)) + 1e-06)
    return (wide * inverse * gain[:, None]).astype(jnp.bfloat16)

def block_sums(weight, acts):
    total_rows = weight.shape[0]
    width = weight.shape[1]
    length = acts.shape[1]
    blocked_w = weight.reshape(total_rows, N_TP, width // N_TP).astype(jnp.float32)
    blocked_a = acts.reshape(N_TP, width // N_TP, length).astype(jnp.float32)
    partials = jnp.einsum('dpc,pcl->pdl', blocked_w, blocked_a)
    rounded = lax.optimization_barrier(partials.astype(jnp.bfloat16))
    return lax.optimization_barrier(jnp.sum(rounded.astype(jnp.float32), axis=0))

def one_sequence(seq, mixer_gain, glu_value, glu_gate, conv_kernel, channel_gain, conv_out, ffn_gain, ffn_gate, ffn_up, ffn_down):
    length = seq.shape[1]
    wide = seq.astype(jnp.float32)
    normed = rms_normalize(wide, mixer_gain)
    value_part = jnp.dot(glu_value.T, normed, preferred_element_type=jnp.float32)
    gate_part = jnp.dot(glu_gate.T, normed, preferred_element_type=jnp.float32)
    gated = (value_part * jax.nn.sigmoid(gate_part)).astype(jnp.float32)
    gated = lax.optimization_barrier(gated.astype(jnp.bfloat16)).astype(jnp.float32)
    padded = jnp.pad(gated, ((0, 0), (KERNEL - 1, 0)))
    taps = conv_kernel.astype(jnp.float32)
    conv_sum = jnp.zeros_like(gated)
    for step in range(KERNEL):
        conv_sum = conv_sum + taps[step][:, None] * padded[:, step:step + length]
    mean_val = lax.optimization_barrier(jnp.mean(conv_sum, axis=0, keepdims=True))
    mean_sq = lax.optimization_barrier(jnp.mean(conv_sum * conv_sum, axis=0, keepdims=True))
    scaled = (conv_sum - mean_val) * lax.rsqrt(mean_sq - mean_val * mean_val + 1e-05) * channel_gain[:, None]
    activated = jax.nn.silu(scaled).astype(jnp.bfloat16)
    mixed_sum = block_sums(conv_out, activated)
    middle = (wide + mixed_sum).astype(jnp.bfloat16)
    middle_wide = middle.astype(jnp.float32)
    normed_two = rms_normalize(middle_wide, ffn_gain)
    gate_val = jnp.dot(ffn_gate.T, normed_two, preferred_element_type=jnp.float32)
    up_val = jnp.dot(ffn_up.T, normed_two, preferred_element_type=jnp.float32)
    hidden = (jax.nn.silu(gate_val) * up_val).astype(jnp.bfloat16)
    ffn_sum = block_sums(ffn_down, hidden)
    return (middle_wide + ffn_sum).astype(jnp.bfloat16)

def reference(stream, mixer_gain, glu_value, glu_gate, conv_kernel, channel_gain, conv_out, ffn_gain, ffn_gate, ffn_up, ffn_down):
    width = stream.shape[0]
    count = stream.shape[1] // TOK_DEV
    seqs = jnp.transpose(stream.reshape(width, count, TOK_DEV), (1, 0, 2))

    def run(seq):
        return one_sequence(seq, mixer_gain, glu_value, glu_gate, conv_kernel, channel_gain, conv_out, ffn_gain, ffn_gate, ffn_up, ffn_down)
    outputs = lax.map(run, seqs)
    return jnp.transpose(outputs, (1, 0, 2)).reshape(width, count * TOK_DEV)
```

```python
import functools

import jax
import jax.numpy as jnp
from jax import lax
from jax.experimental import pallas as pl
from jax.experimental.pallas import tpu as pltpu
from jax.sharding import PartitionSpec as P

MESH = pl.DeviceIdType.MESH
BF, F32 = jnp.bfloat16, jnp.float32
CW, CCW = 0, 1


def dot_nn(a, b):
    return lax.dot_general(a, b, (((1,), (0,)), ((), ())), preferred_element_type=F32)


def dot_nt(a, b):
    return lax.dot_general(a, b, (((1,), (1,)), ((), ())), preferred_element_type=F32)


def kernel(
    nz, nt,
    stream, mixer_gain, conv_kernel, channel_gain, ffn_gain, gv, gg, co, wg, wu, wd,
    out,
    glu, gu, dn, ag1, ag2, nrm, pad, cvt, act, stats, hid, acc, mid,
    pb, rb, sb, cb, pb2, rb2, sb2, cb2,
    loc_sem, zsend, zrecv, ysend, yrecv, ag_send, ag_recv, st_send, st_recv,
    d_send, d_recv, c_send, c_recv,
):
    g, z, t = lax.axis_index("grp"), lax.axis_index("fs"), lax.axis_index("tp")
    gi = lax.rem(g, 2)
    mate = g + 1 - 2 * gi
    core = lax.rem(t, 2)
    x = t // 2
    nx = nt // 2
    twin = t + 1 - 2 * core
    right, left = lax.rem(z + 1, nz), lax.rem(z + nz - 1, nz)
    rows, toks = stream.shape
    width = rows * nt
    srows = gv.shape[0]
    chans = gv.shape[1]
    taps = conv_kernel.shape[0]
    ncw, nccw = nz // 2, nz - 1 - nz // 2

    def at_chip(o):
        return lax.rem(x + o, nx) * 2 + core

    own = pl.ds(pl.multiple_of(z * srows, srows), srows)
    locals_ = [
        pltpu.make_async_copy(gv, glu.at[own, pl.ds(0, chans)], loc_sem.at[0]),
        pltpu.make_async_copy(gg, glu.at[own, pl.ds(chans, chans)], loc_sem.at[1]),
        pltpu.make_async_copy(co, glu.at[own, pl.ds(2 * chans, chans)], loc_sem.at[2]),
        pltpu.make_async_copy(wg, gu.at[0, own, :], loc_sem.at[3]),
        pltpu.make_async_copy(wu, gu.at[1, own, :], loc_sem.at[4]),
        pltpu.make_async_copy(wd, dn.at[own, :], loc_sem.at[5]),
    ]
    for c in locals_:
        c.start()

    barrier = pltpu.get_barrier_semaphore()
    for peer in (right, left):
        pl.semaphore_signal(barrier, inc=1, device_id={"fs": peer}, device_id_type=MESH)
    pl.semaphore_signal(barrier, inc=1, device_id={"grp": mate}, device_id_type=MESH)
    for o in range(1, nt):
        pl.semaphore_signal(
            barrier, inc=1, device_id={"tp": lax.rem(t + o, nt)}, device_id_type=MESH
        )
    ag1[t] = stream[...].T
    for c in locals_:
        c.wait()
    pl.semaphore_wait(barrier, 2 + nt)

    half, quarter = srows // 2, srows // 4

    def slot(p, zz):
        base = zz * srows
        if p < 2:
            return glu.at[pl.ds(pl.multiple_of(base + half * p, half), half), :]
        k = (p - 2) % 4
        r = pl.ds(pl.multiple_of(base + quarter * k, quarter), quarter)
        return gu.at[gi, r, :] if p < 6 else dn.at[r, :]

    def zcopy(p, d, zz, s):
        return pltpu.make_async_remote_copy(
            src_ref=slot(p, zz), dst_ref=slot(p, zz),
            send_sem=zsend.at[d, p], recv_sem=zrecv.at[d, p, s - 1],
            device_id={"fs": right if d == CW else left}, device_id_type=MESH,
        )

    def held(d, s):
        return lax.rem(z - s + nz, nz) if d == CW else lax.rem(z + s, nz)

    def send(p, d, s):
        zcopy(p, d, held(d, s - 1), s).start()

    def ycopy(d, s, whose):
        r = pl.ds(pl.multiple_of(held(d, s) * srows, srows), srows)
        i = d * ncw + s - 1
        return pltpu.make_async_remote_copy(
            src_ref=gu.at[whose, r, :], dst_ref=gu.at[whose, r, :],
            send_sem=ysend, recv_sem=yrecv.at[i],
            device_id={"grp": mate}, device_id_type=MESH,
        )

    def step(pieces, s, dirs, fwd):
        for p in pieces:
            for d in dirs:
                zcopy(p, d, held(d, s), s).wait_recv()
                if d in fwd:
                    send(p, d, s + 1)
        if 5 in pieces:
            for d in dirs:
                ycopy(d, s, gi).start()

    def first(pieces):
        for p in pieces:
            for d in (CW, CCW):
                send(p, d, 1)

    def rounds(pieces, lo, hi):
        top = min(hi, nccw)
        if top > lo:
            @pl.loop(lo, top)
            def _(s):
                step(pieces, s, (CW, CCW), (CW, CCW))
        for s in range(max(lo, nccw), hi):
            step(
                pieces, s,
                (CW, CCW) if s <= nccw else (CW,),
                (CW,) if s < ncw else (),
            )

    def ag_copy(buf, which, block, k, target):
        return pltpu.make_async_remote_copy(
            src_ref=buf.at[block], dst_ref=buf.at[block],
            send_sem=ag_send.at[which, k], recv_sem=ag_recv.at[which, block],
            device_id={"tp": target}, device_id_type=MESH,
        )

    def ag_start(buf, which):
        for k, o in enumerate((2, 1, 3)):
            ag_copy(buf, which, t, k, at_chip(o)).start()
        ag_copy(buf, which, t, 3, twin).start()

    def ag_forward(buf, which, os):
        for o in os:
            b = at_chip(o)
            ag_copy(buf, which, b, 0, twin).wait_recv()
            ag_copy(buf, which, b, 3 + o, twin).start()

    def ag_finish(buf, which):
        ag_copy(buf, which, twin, 0, twin).wait_recv()
        for o in range(1, nx):
            ag_copy(buf, which, lax.rem(x + o, nx) * 2 + 1 - core, 0, twin).wait_recv()

    def ag_drain(buf, which):
        for k in range(4):
            ag_copy(buf, which, t, k, twin).wait_send()
        for o in range(1, nx):
            ag_copy(buf, which, at_chip(o), 3 + o, twin).wait_send()

    tb = toks // 3

    def normalize(buf, gain, b):
        r = pl.ds(b * tb, tb)
        total = jnp.zeros((tb, rows), F32)
        for j in range(nt):
            v = buf[j, r, :].astype(F32)
            total = total + v * v
        inv = lax.rsqrt(jnp.sum(total, axis=1, keepdims=True) / width + 1e-06)
        for j in range(nt):
            v = buf[j, r, :].astype(F32)
            nrm[r, j * rows:(j + 1) * rows] = (
                v * inv * gain[:, j * rows:(j + 1) * rows]
            ).astype(BF)

    order = (2, 1, 3, 0)

    def d_copy(which, o, pbuf, rbuf):
        return pltpu.make_async_remote_copy(
            src_ref=pbuf.at[o], dst_ref=rbuf.at[o],
            send_sem=d_send.at[which, o], recv_sem=d_recv.at[which, o],
            device_id={"tp": twin}, device_id_type=MESH,
        )

    def c_copy(which, o, sbuf, cbuf):
        return pltpu.make_async_remote_copy(
            src_ref=sbuf.at[o - 1], dst_ref=cbuf.at[o - 1],
            send_sem=c_send.at[which, o - 1], recv_sem=c_recv.at[which, o - 1],
            device_id={"tp": at_chip(o)}, device_id_type=MESH,
        )

    def rs_first(which, partial, pbuf, rbuf):
        for o in order:
            td = lax.rem(x + o, nx) * 2 + 1 - core
            pbuf[o] = partial(td).astype(BF)
            d_copy(which, o, pbuf, rbuf).start()

    def rs_second(which, partial, pbuf, rbuf, sbuf, cbuf):
        for o in order:
            mine = partial(at_chip(o))
            d_copy(which, o, pbuf, rbuf).wait_recv()
            both = mine + rbuf[o].astype(F32)
            if o:
                sbuf[o - 1] = both.astype(BF)
                c_copy(which, o, sbuf, cbuf).start()
            else:
                acc[...] = both

    def rs_third(which, sbuf, cbuf):
        total = acc[...]
        for o in order[:3]:
            c_copy(which, o, sbuf, cbuf).wait_recv()
            total = total + cbuf[o - 1].astype(F32)
        return total

    def rs_drain(which, pbuf, rbuf, sbuf, cbuf):
        for o in order:
            d_copy(which, o, pbuf, rbuf).wait_send()
            if o:
                c_copy(which, o, sbuf, cbuf).wait_send()

    def out_rows(td):
        return pl.ds(pl.multiple_of(td * rows, rows), rows)

    early = (0, 1, 2, 3, 4, 5)
    late = (6, 7, 8, 9)
    first((0, 1))
    ag_start(ag1, 0)
    first((2, 3, 4, 5))
    rounds(early, 1, 4)
    ag_forward(ag1, 0, (1, 3))
    rounds(early, 4, 5)
    ag_forward(ag1, 0, (2,))
    rounds(early, 5, 7)
    ag_finish(ag1, 0)
    normalize(ag1, mixer_gain, 0)
    rounds(early, 7, 8)
    normalize(ag1, mixer_gain, 1)
    rounds(early, 8, 9)
    normalize(ag1, mixer_gain, 2)
    pad[0:32, :] = jnp.zeros((32, chans), F32)
    rounds(early, 9, nz // 2)
    first(late)
    rounds(early, nz // 2, nz // 2 + 1)

    both = dot_nn(nrm[...], glu[:, 0:2 * chans])
    gated = both[:, :chans] * jax.nn.sigmoid(both[:, chans:])
    pad[32:32 + toks, :] = gated.astype(BF).astype(F32)
    rounds(late, 1, 2)
    lanes = pl.ds(pl.multiple_of(t * chans, chans), chans)
    kern = conv_kernel[:, lanes].astype(F32)
    nb = 6
    bt = toks // nb
    for b in range(nb):
        total = jnp.zeros((bt, chans), F32)
        for k in range(taps):
            lo = b * bt + 32 - (taps - 1) + k
            total = total + kern[k:k + 1, :] * pad[lo:lo + bt, :]
        cvt[b * bt:(b + 1) * bt, :] = total
    flipped = cvt[...].T
    stats[t, 0:1, :] = jnp.sum(flipped, axis=0, keepdims=True)
    stats[t, 1:2, :] = jnp.sum(flipped * flipped, axis=0, keepdims=True)

    def st_copy(o, src, target):
        return pltpu.make_async_remote_copy(
            src_ref=stats.at[src], dst_ref=stats.at[src],
            send_sem=st_send.at[o], recv_sem=st_recv.at[src],
            device_id={"tp": target}, device_id_type=MESH,
        )

    for o in range(1, nt):
        st_copy(o, t, lax.rem(t + o, nt)).start()
    rounds(late, 2, 3)
    for o in range(1, nt):
        st_copy(o, lax.rem(t + o, nt), lax.rem(t + o, nt)).wait_recv()
    total = stats[0]
    for j in range(1, nt):
        total = total + stats[j]
    total = total / (chans * nt)
    mean, msq = total[0:1], total[1:2]
    inv = lax.rsqrt(msq - mean * mean + 1e-05)
    cols = jnp.concatenate([mean, inv, jnp.zeros((6, toks), F32)], axis=0).T
    cgain = channel_gain[:, lanes]
    scaled = (cvt[...] - cols[:, 0:1]) * cols[:, 1:2] * cgain
    act[...] = (scaled * jax.nn.sigmoid(scaled)).astype(BF)

    def mixed_part(td):
        return dot_nt(glu[out_rows(td), 2 * chans:3 * chans], act[...])

    rs_first(0, mixed_part, pb, rb)
    rounds(late, 3, 4)
    rs_second(0, mixed_part, pb, rb, sb, cb)
    rounds(late, 4, 7)
    middle = (stream[...].astype(F32) + rs_third(0, sb, cb)).astype(BF)
    mid[...] = middle
    ag2[t] = middle.T
    ag_start(ag2, 1)
    rounds(late, 7, 9)
    ag_forward(ag2, 1, (1, 3))
    rounds(late, 9, 10)
    ag_forward(ag2, 1, (2,))
    rounds(late, 10, 11)
    ag_finish(ag2, 1)
    for b in range(3):
        normalize(ag2, ffn_gain, b)
        rounds(late, 11 + b, 12 + b)

    for d, n in ((CW, ncw), (CCW, nccw)):
        @pl.loop(1, n + 1)
        def _(s):
            ycopy(d, s, 1 - gi).wait_recv()

    ff = gu.shape[2]
    for b, lo in enumerate(range(0, ff, 256)):
        hi = min(lo + 256, ff)
        gate = dot_nn(nrm[...], gu[0, :, lo:hi])
        up = dot_nn(nrm[...], gu[1, :, lo:hi])
        hid[:, lo:hi] = (gate * jax.nn.sigmoid(gate) * up).astype(BF)
        if b < 2:
            rounds(late, 14 + b, 15 + b)
    rounds(late, 16, nz // 2 + 1)

    def ffn_part(td):
        return dot_nt(dn[out_rows(td), :], hid[...])

    rs_first(1, ffn_part, pb2, rb2)
    rs_second(1, ffn_part, pb2, rb2, sb2, cb2)

    for p in early + late:
        for d, n in ((CW, ncw), (CCW, nccw)):
            if p < 2:
                ref = glu.at[pl.ds(0, n * half), :]
            elif p < 6:
                ref = gu.at[0, pl.ds(0, n * quarter), :]
            else:
                ref = dn.at[pl.ds(0, n * quarter), :]
            pltpu.make_async_copy(ref, ref, zsend.at[d, p]).wait()
    ref = gu.at[0, pl.ds(0, (nz - 1) * srows), :]
    pltpu.make_async_copy(ref, ref, ysend).wait()
    ag_drain(ag1, 0)
    ag_drain(ag2, 1)
    for o in range(1, nt):
        st_copy(o, t, twin).wait_send()
    rs_drain(0, pb, rb, sb, cb)

    out[...] = (mid[...].astype(F32) + rs_third(1, sb2, cb2)).astype(BF)
    rs_drain(1, pb2, rb2, sb2, cb2)


def solution(mesh):
    nz, nt = mesh.shape["fs"], mesh.shape["tp"]

    def on_device(
        stream, mixer_gain, glu_value, glu_gate, conv_kernel, channel_gain,
        conv_out, ffn_gain, ffn_gate, ffn_up, ffn_down,
    ):
        rows, toks = stream.shape
        srows, chans = glu_value.shape
        ff = ffn_gate.shape[1]
        width = rows * nt
        nx = nt // 2
        vm = pl.BlockSpec(memory_space=pltpu.VMEM)
        hbm = pl.BlockSpec(memory_space=pl.ANY)
        dma = pltpu.SemaphoreType.DMA
        blocks = [
            pltpu.VMEM((nx, rows, toks), BF),
            pltpu.VMEM((nx, rows, toks), BF),
            pltpu.VMEM((nx - 1, rows, toks), BF),
            pltpu.VMEM((nx - 1, rows, toks), BF),
        ]
        return pl.pallas_call(
            functools.partial(kernel, nz, nt),
            out_shape=jax.ShapeDtypeStruct((rows, toks), BF),
            in_specs=[vm] * 5 + [hbm] * 6,
            out_specs=vm,
            scratch_shapes=[
                pltpu.VMEM((width, 3 * chans), BF),
                pltpu.VMEM((2, width, ff), BF),
                pltpu.VMEM((width, ff), BF),
                pltpu.VMEM((nt, toks, rows), BF),
                pltpu.VMEM((nt, toks, rows), BF),
                pltpu.VMEM((toks, width), BF),
                pltpu.VMEM((toks + 32, chans), F32),
                pltpu.VMEM((toks, chans), F32),
                pltpu.VMEM((toks, chans), BF),
                pltpu.VMEM((nt, 2, toks), F32),
                pltpu.VMEM((toks, ff), BF),
                pltpu.VMEM((rows, toks), F32),
                pltpu.VMEM((rows, toks), BF),
                *blocks, *blocks,
                dma((6,)),
                dma((2, 10)),
                dma((2, 10, nz // 2)),
                dma,
                dma((nz,)),
                dma((2, 4 + nx - 1)),
                dma((2, nt)),
                dma((nt,)),
                dma((nt,)),
                dma((2, nx)),
                dma((2, nx)),
                dma((2, nx - 1)),
                dma((2, nx - 1)),
            ],
            compiler_params=pltpu.CompilerParams(collective_id=0, has_side_effects=True),
        )(
            stream, mixer_gain[None, :], conv_kernel, channel_gain[None, :],
            ffn_gain[None, :], glu_value, glu_gate, conv_out, ffn_gate, ffn_up, ffn_down,
        )

    weight = P("fs", "tp")
    in_specs = (
        P("tp", ("grp", "fs")), P(), weight, weight, P(), P(), weight, P(),
        weight, weight, weight,
    )
    return jax.shard_map(
        on_device, mesh=mesh, in_specs=in_specs,
        out_specs=P("tp", ("grp", "fs")), check_vma=False,
    )
```

```python
import functools

import jax
import jax.numpy as jnp
from jax import lax
from jax.experimental import pallas as pl
from jax.experimental.pallas import tpu as pltpu
from jax.sharding import PartitionSpec as P

MESH = pl.DeviceIdType.MESH
BF, F32 = jnp.bfloat16, jnp.float32
CW, CCW = 0, 1
PLACES = (0, 0, 0, 3, 3, 6, 18, 27, 28, 30, 31)


def dot_nn(a, b):
    return lax.dot_general(a, b, (((1,), (0,)), ((), ())), preferred_element_type=F32)


def dot_nt(a, b):
    return lax.dot_general(a, b, (((1,), (1,)), ((), ())), preferred_element_type=F32)


def kernel(
    nz, nt,
    stream, mixer_gain, conv_kernel, channel_gain, ffn_gain, gv, gg, co, wg, wu, wd,
    out,
    glu, gu, dn, tail, ag1, ag2, nrm, pad, cvt, act, stats, hid, acc, mid,
    pb, rb, sb, cb, pb2, rb2, sb2, cb2,
    loc_sem, zsend, zrecv, ysend, yrecv, ytsend, ytrecv, ag_send, ag_recv, st_send, st_recv,
    d_send, d_recv, c_send, c_recv,
):
    g, z, t = lax.axis_index("grp"), lax.axis_index("fs"), lax.axis_index("tp")
    gi = lax.rem(g, 2)
    mate = g + 1 - 2 * gi
    core = lax.rem(t, 2)
    x = t // 2
    nx = nt // 2
    twin = t + 1 - 2 * core
    right, left = lax.rem(z + 1, nz), lax.rem(z + nz - 1, nz)
    rows, toks = stream.shape
    width = rows * nt
    srows = gv.shape[0]
    chans = gv.shape[1]
    taps = conv_kernel.shape[0]
    ncw, nccw = nz // 2, nz - 1 - nz // 2

    def at_chip(o):
        return lax.rem(x + o, nx) * 2 + core

    own = pl.ds(pl.multiple_of(z * srows, srows), srows)
    main = gu.shape[2]
    locals_ = [
        pltpu.make_async_copy(gv, glu.at[own, pl.ds(0, chans)], loc_sem.at[0]),
        pltpu.make_async_copy(gg, glu.at[own, pl.ds(chans, chans)], loc_sem.at[1]),
        pltpu.make_async_copy(co, glu.at[own, pl.ds(2 * chans, chans)], loc_sem.at[2]),
        pltpu.make_async_copy(wg.at[:, pl.ds(0, main)], gu.at[0, own, :], loc_sem.at[3]),
        pltpu.make_async_copy(wu.at[:, pl.ds(0, main)], gu.at[1, own, :], loc_sem.at[4]),
        pltpu.make_async_copy(wd.at[:, pl.ds(0, main)], dn.at[own, :], loc_sem.at[5]),
    ]
    for c in locals_:
        c.start()
    for i, w in enumerate((wg, wu)):
        tail[i, own, :] = jnp.concatenate([w[:, main:], wd[:, main:]], axis=1)

    barrier = pltpu.get_barrier_semaphore()
    for peer in (right, left):
        pl.semaphore_signal(barrier, inc=1, device_id={"fs": peer}, device_id_type=MESH)
    pl.semaphore_signal(barrier, inc=1, device_id={"grp": mate}, device_id_type=MESH)
    for o in range(1, nt):
        pl.semaphore_signal(
            barrier, inc=1, device_id={"tp": lax.rem(t + o, nt)}, device_id_type=MESH
        )
    for c in locals_:
        c.wait()
    pl.semaphore_wait(barrier, 2 + nt)

    half, quarter = srows // 2, srows // 4

    def slot(p, zz):
        base = zz * srows
        if p < 2:
            return glu.at[pl.ds(pl.multiple_of(base + half * p, half), half), :]
        if p == 10:
            return tail.at[gi, pl.ds(pl.multiple_of(base, srows), srows), :]
        k = (p - 2) % 4
        r = pl.ds(pl.multiple_of(base + quarter * k, quarter), quarter)
        return gu.at[gi, r, :] if p < 6 else dn.at[r, :]

    def zcopy(p, d, zz, s):
        return pltpu.make_async_remote_copy(
            src_ref=slot(p, zz), dst_ref=slot(p, zz),
            send_sem=zsend.at[d, p], recv_sem=zrecv.at[d, p, s - 1],
            device_id={"fs": right if d == CW else left}, device_id_type=MESH,
        )

    def held(d, s):
        return lax.rem(z - s + nz, nz) if d == CW else lax.rem(z + s, nz)

    def send(p, d, s):
        zcopy(p, d, held(d, s - 1), s).start()

    def ycopy(d, s, whose):
        r = pl.ds(pl.multiple_of(held(d, s) * srows, srows), srows)
        i = d * ncw + s - 1
        return pltpu.make_async_remote_copy(
            src_ref=gu.at[whose, r, :], dst_ref=gu.at[whose, r, :],
            send_sem=ysend, recv_sem=yrecv.at[i],
            device_id={"grp": mate}, device_id_type=MESH,
        )

    def ytcopy(d, s, whose):
        r = pl.ds(pl.multiple_of(held(d, s) * srows, srows), srows)
        return pltpu.make_async_remote_copy(
            src_ref=tail.at[whose, r, :], dst_ref=tail.at[whose, r, :],
            send_sem=ytsend, recv_sem=ytrecv.at[d * ncw + s - 1],
            device_id={"grp": mate}, device_id_type=MESH,
        )

    def step(pieces, s, dirs, fwd):
        for p in pieces:
            for d in dirs:
                zcopy(p, d, held(d, s), s).wait_recv()
                if d in fwd:
                    send(p, d, s + 1)
        if 5 in pieces:
            for d in dirs:
                ycopy(d, s, gi).start()
                ytcopy(d, s, gi).start()

    glus, ms, ds = (0, 1), (2, 3, 4, 5, 10), (6, 7, 8, 9)

    def first(pieces):
        for p in pieces:
            for d in (CW, CCW):
                send(p, d, 1)

    def far_way(p):
        return CCW if p in ds else CW

    def whole(s, pieces):
        step(pieces, s, (CW, CCW), (CW, CCW))

    def last(s, pieces):
        far = far_way(pieces[0])
        dirs = (CW, CCW) if s <= nccw else (far,)
        step(pieces, s, dirs, (far,) if s < ncw else ())

    def any_step(s, pieces):
        (whole if s < nccw else last)(s, pieces)

    def unit(u):
        if u <= ncw:
            any_step(u, glus)
        if u % 2:
            any_step((u + 1) // 2, ms)
        else:
            any_step(u // 2, ds)

    def units(lo, hi):
        @pl.loop((lo + 1) // 2, (hi + 1) // 2)
        def _(v):
            whole(2 * v - 1, glus)
            whole(v, ms)
            whole(2 * v, glus)
            whole(v, ds)

    def ag_copy(buf, which, block, k, target):
        return pltpu.make_async_remote_copy(
            src_ref=buf.at[block], dst_ref=buf.at[block],
            send_sem=ag_send.at[which, k], recv_sem=ag_recv.at[which, block],
            device_id={"tp": target}, device_id_type=MESH,
        )

    def ag_start(buf, which):
        for k, o in enumerate((2, 1, 3)):
            ag_copy(buf, which, t, k, at_chip(o)).start()
        ag_copy(buf, which, t, 3, twin).start()

    def ag_forward(buf, which, os):
        for o in os:
            b = at_chip(o)
            ag_copy(buf, which, b, 0, twin).wait_recv()
            ag_copy(buf, which, b, 3 + o, twin).start()

    def ag_finish(buf, which):
        ag_copy(buf, which, twin, 0, twin).wait_recv()
        for o in range(1, nx):
            ag_copy(buf, which, lax.rem(x + o, nx) * 2 + 1 - core, 0, twin).wait_recv()

    def ag_drain(buf, which):
        for k in range(4):
            ag_copy(buf, which, t, k, twin).wait_send()
        for o in range(1, nx):
            ag_copy(buf, which, at_chip(o), 3 + o, twin).wait_send()

    tb = toks // 3

    def normalize(buf, gain, b):
        r = pl.ds(b * tb, tb)
        total = jnp.zeros((tb, rows), F32)
        for j in range(nt):
            v = buf[j, r, :].astype(F32)
            total = total + v * v
        inv = lax.rsqrt(jnp.sum(total, axis=1, keepdims=True) / width + 1e-06)
        for j in range(nt):
            v = buf[j, r, :].astype(F32)
            nrm[r, j * rows:(j + 1) * rows] = (
                v * inv * gain[:, j * rows:(j + 1) * rows]
            ).astype(BF)

    order = (2, 1, 3, 0)

    def d_copy(which, o, pbuf, rbuf):
        return pltpu.make_async_remote_copy(
            src_ref=pbuf.at[o], dst_ref=rbuf.at[o],
            send_sem=d_send.at[which, o], recv_sem=d_recv.at[which, o],
            device_id={"tp": twin}, device_id_type=MESH,
        )

    def c_copy(which, o, sbuf, cbuf):
        return pltpu.make_async_remote_copy(
            src_ref=sbuf.at[o - 1], dst_ref=cbuf.at[o - 1],
            send_sem=c_send.at[which, o - 1], recv_sem=c_recv.at[which, o - 1],
            device_id={"tp": at_chip(o)}, device_id_type=MESH,
        )

    def rs_first(which, partial, pbuf, rbuf):
        for o in order:
            td = lax.rem(x + o, nx) * 2 + 1 - core
            pbuf[o] = partial(td).astype(BF)
            d_copy(which, o, pbuf, rbuf).start()

    def rs_second(which, partial, pbuf, rbuf, sbuf, cbuf):
        for o in order:
            mine = partial(at_chip(o))
            d_copy(which, o, pbuf, rbuf).wait_recv()
            both = mine + rbuf[o].astype(F32)
            if o:
                sbuf[o - 1] = both.astype(BF)
                c_copy(which, o, sbuf, cbuf).start()
            else:
                acc[...] = both

    def rs_third(which, sbuf, cbuf):
        total = acc[...]
        for o in order[:3]:
            c_copy(which, o, sbuf, cbuf).wait_recv()
            total = total + cbuf[o - 1].astype(F32)
        return total

    def rs_drain(which, pbuf, rbuf, sbuf, cbuf):
        for o in order:
            d_copy(which, o, pbuf, rbuf).wait_send()
            if o:
                c_copy(which, o, sbuf, cbuf).wait_send()

    def out_rows(td):
        return pl.ds(pl.multiple_of(td * rows, rows), rows)

    first(glus)
    first(ms)
    first(ds)
    ag1[t] = stream[...].T
    ag_start(ag1, 0)
    units(1, 5)
    ag_forward(ag1, 0, (1, 3))
    unit(5)
    ag_forward(ag1, 0, (2,))
    unit(6)
    ag_finish(ag1, 0)
    normalize(ag1, mixer_gain, 0)
    unit(7)
    normalize(ag1, mixer_gain, 1)
    unit(8)
    normalize(ag1, mixer_gain, 2)
    pad[0:32, :] = jnp.zeros((32, chans), F32)
    units(9, 15)
    unit(15)
    unit(16)

    lanes = pl.ds(pl.multiple_of(t * chans, chans), chans)
    nb = 6
    bt = toks // nb

    def st_copy(o, src, target):
        return pltpu.make_async_remote_copy(
            src_ref=stats.at[src], dst_ref=stats.at[src],
            send_sem=st_send.at[o], recv_sem=st_recv.at[src],
            device_id={"tp": target}, device_id_type=MESH,
        )

    def gated():
        both = dot_nn(nrm[...], glu[:, 0:2 * chans])
        value = both[:, :chans] * jax.nn.sigmoid(both[:, chans:])
        pad[32:32 + toks, :] = value.astype(BF).astype(F32)

    def convolve(blocks):
        kern = conv_kernel[:, lanes].astype(F32)
        for b in blocks:
            total = jnp.zeros((bt, chans), F32)
            for k in range(taps):
                lo = b * bt + 32 - (taps - 1) + k
                total = total + kern[k:k + 1, :] * pad[lo:lo + bt, :]
            cvt[b * bt:(b + 1) * bt, :] = total

    def send_stats():
        flipped = cvt[...].T
        stats[t, 0:1, :] = jnp.sum(flipped, axis=0, keepdims=True)
        stats[t, 1:2, :] = jnp.sum(flipped * flipped, axis=0, keepdims=True)
        for o in range(1, nt):
            st_copy(o, t, lax.rem(t + o, nt)).start()

    def mixed_part(td):
        return dot_nt(glu[out_rows(td), 2 * chans:3 * chans], act[...])

    def activate():
        for o in range(1, nt):
            st_copy(o, lax.rem(t + o, nt), lax.rem(t + o, nt)).wait_recv()
        total = stats[0]
        for j in range(1, nt):
            total = total + stats[j]
        total = total / (chans * nt)
        mean, msq = total[0:1], total[1:2]
        inv = lax.rsqrt(msq - mean * mean + 1e-05)
        cols = jnp.concatenate([mean, inv, jnp.zeros((6, toks), F32)], axis=0).T
        scaled = (cvt[...] - cols[:, 0:1]) * cols[:, 1:2] * channel_gain[:, lanes]
        act[...] = (scaled * jax.nn.sigmoid(scaled)).astype(BF)

    def middle():
        mid[...] = (stream[...].astype(F32) + rs_third(0, sb, cb)).astype(BF)
        ag2[t] = mid[...].T
        ag_start(ag2, 1)

    def hand_over():
        for d, n in ((CW, ncw), (CCW, nccw)):
            @pl.loop(1, n + 1)
            def _(s):
                ycopy(d, s, 1 - gi).wait_recv()
                ytcopy(d, s, 1 - gi).wait_recv()

    def hide():
        rest = tail.shape[2] // 2
        for lo in range(0, main, 256):
            hi = min(lo + 256, main)
            gate = dot_nn(nrm[...], gu[0, :, lo:hi])
            up = dot_nn(nrm[...], gu[1, :, lo:hi])
            hid[:, lo:hi] = (gate * jax.nn.sigmoid(gate) * up).astype(BF)
        gate, up = dot_nn(nrm[...], tail[0]), dot_nn(nrm[...], tail[1])
        gate, up = gate[:, :rest], up[:, :rest]
        ends = gate * jax.nn.sigmoid(gate) * up
        hid[:, main:] = jnp.concatenate([jnp.zeros_like(ends), ends], axis=1).astype(BF)

    events = (
        gated,
        lambda: convolve(range(nb // 2)),
        lambda: [convolve(range(nb // 2, nb)), send_stats()],
        activate,
        lambda: rs_first(0, mixed_part, pb, rb),
        lambda: rs_second(0, mixed_part, pb, rb, sb, cb),
        middle,
        lambda: ag_forward(ag2, 1, (1, 3)),
        lambda: ag_forward(ag2, 1, (2,)),
        lambda: ag_finish(ag2, 1),
        lambda: [normalize(ag2, ffn_gain, b) for b in range(3)],
    )
    for k in range(2 * (nz - 16) + 1):
        if k:
            u = 16 + (k + 1) // 2
            pieces = ms if u % 2 else ds
            any_step((u + 1) // 2, pieces[:2] if k % 2 else pieces[2:])
        for at, event in zip(PLACES, events):
            if at == k:
                event()
    hand_over()
    hide()

    def ffn_part(td):
        r = out_rows(td)
        return dot_nt(dn[r, :], hid[:, :main]) + dot_nt(tail[0, r, :], hid[:, main:])

    rs_first(1, ffn_part, pb2, rb2)
    rs_second(1, ffn_part, pb2, rb2, sb2, cb2)

    for p in glus + ms + ds:
        for d in (CW, CCW):
            n = ncw if d == far_way(p) else nccw
            if p < 2:
                ref = glu.at[pl.ds(0, n * half), :]
            elif p < 6:
                ref = gu.at[0, pl.ds(0, n * quarter), :]
            elif p < 10:
                ref = dn.at[pl.ds(0, n * quarter), :]
            else:
                ref = tail.at[0, pl.ds(0, n * srows), :]
            pltpu.make_async_copy(ref, ref, zsend.at[d, p]).wait()
    ref = gu.at[0, pl.ds(0, (nz - 1) * srows), :]
    pltpu.make_async_copy(ref, ref, ysend).wait()
    ref = tail.at[0, pl.ds(0, (nz - 1) * srows), :]
    pltpu.make_async_copy(ref, ref, ytsend).wait()
    ag_drain(ag1, 0)
    ag_drain(ag2, 1)
    for o in range(1, nt):
        st_copy(o, t, twin).wait_send()
    rs_drain(0, pb, rb, sb, cb)

    out[...] = (mid[...].astype(F32) + rs_third(1, sb2, cb2)).astype(BF)
    rs_drain(1, pb2, rb2, sb2, cb2)


def solution(mesh):
    nz, nt = mesh.shape["fs"], mesh.shape["tp"]

    def on_device(
        stream, mixer_gain, glu_value, glu_gate, conv_kernel, channel_gain,
        conv_out, ffn_gain, ffn_gate, ffn_up, ffn_down,
    ):
        rows, toks = stream.shape
        srows, chans = glu_value.shape
        ff = ffn_gate.shape[1]
        main = ff // 128 * 128
        width = rows * nt
        nx = nt // 2
        vm = pl.BlockSpec(memory_space=pltpu.VMEM)
        hbm = pl.BlockSpec(memory_space=pl.ANY)
        dma = pltpu.SemaphoreType.DMA
        blocks = [
            pltpu.VMEM((nx, rows, toks), BF),
            pltpu.VMEM((nx, rows, toks), BF),
            pltpu.VMEM((nx - 1, rows, toks), BF),
            pltpu.VMEM((nx - 1, rows, toks), BF),
        ]
        return pl.pallas_call(
            functools.partial(kernel, nz, nt),
            out_shape=jax.ShapeDtypeStruct((rows, toks), BF),
            in_specs=[vm] * 5 + [hbm] * 3 + [vm] * 3,
            out_specs=vm,
            scratch_shapes=[
                pltpu.VMEM((width, 3 * chans), BF),
                pltpu.VMEM((2, width, main), BF),
                pltpu.VMEM((width, main), BF),
                pltpu.VMEM((2, width, 2 * (ff - main)), BF),
                pltpu.VMEM((nt, toks, rows), BF),
                pltpu.VMEM((nt, toks, rows), BF),
                pltpu.VMEM((toks, width), BF),
                pltpu.VMEM((toks + 32, chans), F32),
                pltpu.VMEM((toks, chans), F32),
                pltpu.VMEM((toks, chans), BF),
                pltpu.VMEM((nt, 2, toks), F32),
                pltpu.VMEM((toks, main + 2 * (ff - main)), BF),
                pltpu.VMEM((rows, toks), F32),
                pltpu.VMEM((rows, toks), BF),
                *blocks, *blocks,
                dma((6,)),
                dma((2, 11)),
                dma((2, 11, nz // 2)),
                dma,
                dma((nz,)),
                dma,
                dma((nz,)),
                dma((2, 4 + nx - 1)),
                dma((2, nt)),
                dma((nt,)),
                dma((nt,)),
                dma((2, nx)),
                dma((2, nx)),
                dma((2, nx - 1)),
                dma((2, nx - 1)),
            ],
            compiler_params=pltpu.CompilerParams(collective_id=0, has_side_effects=True),
        )(
            stream, mixer_gain[None, :], conv_kernel, channel_gain[None, :],
            ffn_gain[None, :], glu_value, glu_gate, conv_out, ffn_gate, ffn_up, ffn_down,
        )

    weight = P("fs", "tp")
    in_specs = (
        P("tp", ("grp", "fs")), P(), weight, weight, P(), P(), weight, P(),
        weight, weight, weight,
    )
    return jax.shard_map(
        on_device, mesh=mesh, in_specs=in_specs,
        out_specs=P("tp", ("grp", "fs")), check_vma=False,
    )
```

```python
import functools

import jax
import jax.numpy as jnp
from jax import lax
from jax.experimental import pallas as pl
from jax.experimental.pallas import tpu as pltpu
from jax.sharding import PartitionSpec as P

MESH = pl.DeviceIdType.MESH
BF, F32 = jnp.bfloat16, jnp.float32
CW, CCW = 0, 1
PLACES = (0, 0, 0, 3, 3, 6, 18, 27, 28, 29, 30, 30, 30)
LEAD = 1


def dot_nn(a, b):
    return lax.dot_general(a, b, (((1,), (0,)), ((), ())), preferred_element_type=F32)


def dot_nt(a, b):
    return lax.dot_general(a, b, (((1,), (1,)), ((), ())), preferred_element_type=F32)


def kernel(
    nz, nt,
    stream, mixer_gain, conv_kernel, channel_gain, ffn_gain, gv, gg, co, wg, wu, wd,
    out,
    glu, gu, dn, tail, ag1, ag2, nrm, pad, cvt, act, stats, hid, acc, mid,
    pb, rb, sb, cb, pb2, rb2, sb2, cb2,
    loc_sem, zsend, zrecv, ysend, yrecv, ytsend, ytrecv, ag_send, ag_recv, st_send, st_recv,
    d_send, d_recv, c_send, c_recv,
):
    g, z, t = lax.axis_index("grp"), lax.axis_index("fs"), lax.axis_index("tp")
    gi = lax.rem(g, 2)
    mate = g + 1 - 2 * gi
    core = lax.rem(t, 2)
    x = t // 2
    nx = nt // 2
    twin = t + 1 - 2 * core
    right, left = lax.rem(z + 1, nz), lax.rem(z + nz - 1, nz)
    rows, toks = stream.shape
    width = rows * nt
    srows = gv.shape[0]
    chans = gv.shape[1]
    taps = conv_kernel.shape[0]
    ncw, nccw = nz // 2, nz - 1 - nz // 2

    def at_chip(o):
        return lax.rem(x + o, nx) * 2 + core

    barrier = pltpu.get_barrier_semaphore()
    for peer in (right, left):
        pl.semaphore_signal(barrier, inc=1, device_id={"fs": peer}, device_id_type=MESH)
    pl.semaphore_signal(barrier, inc=1, device_id={"grp": mate}, device_id_type=MESH)
    for o in range(1, nt):
        pl.semaphore_signal(
            barrier, inc=1, device_id={"tp": lax.rem(t + o, nt)}, device_id_type=MESH
        )
    own = pl.ds(pl.multiple_of(z * srows, srows), srows)
    main = gu.shape[2]
    locals_ = [
        pltpu.make_async_copy(gv, glu.at[own, pl.ds(0, chans)], loc_sem.at[0]),
        pltpu.make_async_copy(gg, glu.at[own, pl.ds(chans, chans)], loc_sem.at[1]),
        pltpu.make_async_copy(co, glu.at[own, pl.ds(2 * chans, chans)], loc_sem.at[2]),
        pltpu.make_async_copy(wg.at[:, pl.ds(0, main)], gu.at[0, own, :], loc_sem.at[3]),
        pltpu.make_async_copy(wu.at[:, pl.ds(0, main)], gu.at[1, own, :], loc_sem.at[4]),
        pltpu.make_async_copy(wd.at[:, pl.ds(0, main)], dn.at[own, :], loc_sem.at[5]),
    ]
    for c in locals_:
        c.start()
    for c in locals_[:3]:
        c.wait()
    pl.semaphore_wait(barrier, 2 + nt)

    half, quarter = srows // 2, srows // 4

    def slot(p, zz):
        base = zz * srows
        if p < 2:
            return glu.at[pl.ds(pl.multiple_of(base + half * p, half), half), :]
        if p == 10:
            return tail.at[gi, pl.ds(pl.multiple_of(base, srows), srows), :]
        k = (p - 2) % 4
        r = pl.ds(pl.multiple_of(base + quarter * k, quarter), quarter)
        return gu.at[gi, r, :] if p < 6 else dn.at[r, :]

    def zcopy(p, d, zz, s):
        return pltpu.make_async_remote_copy(
            src_ref=slot(p, zz), dst_ref=slot(p, zz),
            send_sem=zsend.at[d, p], recv_sem=zrecv.at[d, p, s - 1],
            device_id={"fs": right if d == CW else left}, device_id_type=MESH,
        )

    def held(d, s):
        return lax.rem(z - s + nz, nz) if d == CW else lax.rem(z + s, nz)

    def send(p, d, s):
        zcopy(p, d, held(d, s - 1), s).start()

    def ycopy(d, s, whose):
        r = pl.ds(pl.multiple_of(held(d, s) * srows, srows), srows)
        i = d * ncw + s - 1
        return pltpu.make_async_remote_copy(
            src_ref=gu.at[whose, r, :], dst_ref=gu.at[whose, r, :],
            send_sem=ysend, recv_sem=yrecv.at[i],
            device_id={"grp": mate}, device_id_type=MESH,
        )

    def ytcopy(d, s, whose):
        r = pl.ds(pl.multiple_of(held(d, s) * srows, srows), srows)
        return pltpu.make_async_remote_copy(
            src_ref=tail.at[whose, r, :], dst_ref=tail.at[whose, r, :],
            send_sem=ytsend, recv_sem=ytrecv.at[d * ncw + s - 1],
            device_id={"grp": mate}, device_id_type=MESH,
        )

    def step(pieces, s, dirs, fwd):
        for p in pieces:
            for d in dirs:
                zcopy(p, d, held(d, s), s).wait_recv()
                if d in fwd:
                    send(p, d, s + 1)
        if 5 in pieces:
            for d in dirs:
                ycopy(d, s, gi).start()
                ytcopy(d, s, gi).start()

    glus, ms, ds = (0, 1), (2, 3, 4, 5, 10), (6, 7, 8, 9)

    def first(pieces):
        for p in pieces:
            for d in (CW, CCW):
                send(p, d, 1)

    def far_way(p):
        return CCW if p in ds else CW

    def whole(s, pieces):
        step(pieces, s, (CW, CCW), (CW, CCW))

    def last(s, pieces):
        far = far_way(pieces[0])
        dirs = (CW, CCW) if s <= nccw else (far,)
        step(pieces, s, dirs, (far,) if s < ncw else ())

    def any_step(s, pieces):
        (whole if s < nccw else last)(s, pieces)

    def unit(u):
        if u <= ncw:
            any_step(u, glus)
        if u % 2:
            any_step((u + 1) // 2, ms)
        else:
            any_step(u // 2, ds)

    def units(lo, hi):
        @pl.loop((lo + 1) // 2, (hi + 1) // 2)
        def _(v):
            whole(2 * v - 1, glus)
            whole(v, ms)
            whole(2 * v, glus)
            whole(v, ds)

    def ag_copy(buf, which, block, k, target):
        return pltpu.make_async_remote_copy(
            src_ref=buf.at[block], dst_ref=buf.at[block],
            send_sem=ag_send.at[which, k], recv_sem=ag_recv.at[which, block],
            device_id={"tp": target}, device_id_type=MESH,
        )

    def ag_start(buf, which):
        for k, o in enumerate((2, 1, 3)):
            ag_copy(buf, which, t, k, at_chip(o)).start()
        ag_copy(buf, which, t, 3, twin).start()

    def ag_forward(buf, which, os):
        for o in os:
            b = at_chip(o)
            ag_copy(buf, which, b, 0, twin).wait_recv()
            ag_copy(buf, which, b, 3 + o, twin).start()

    def ag_finish(buf, which):
        ag_copy(buf, which, twin, 0, twin).wait_recv()
        for o in range(1, nx):
            ag_copy(buf, which, lax.rem(x + o, nx) * 2 + 1 - core, 0, twin).wait_recv()

    def ag_drain(buf, which):
        for k in range(4):
            ag_copy(buf, which, t, k, twin).wait_send()
        for o in range(1, nx):
            ag_copy(buf, which, at_chip(o), 3 + o, twin).wait_send()

    tb = toks // 3

    def normalize(buf, gain, b):
        r = pl.ds(b * tb, tb)
        total = jnp.zeros((tb, rows), F32)
        for j in range(nt):
            v = buf[j, r, :].astype(F32)
            total = total + v * v
        inv = lax.rsqrt(jnp.sum(total, axis=1, keepdims=True) / width + 1e-06)
        for j in range(nt):
            v = buf[j, r, :].astype(F32)
            nrm[r, j * rows:(j + 1) * rows] = (
                v * inv * gain[:, j * rows:(j + 1) * rows]
            ).astype(BF)

    order = (2, 1, 3, 0)

    def d_copy(which, o, pbuf, rbuf):
        return pltpu.make_async_remote_copy(
            src_ref=pbuf.at[o], dst_ref=rbuf.at[o],
            send_sem=d_send.at[which, o], recv_sem=d_recv.at[which, o],
            device_id={"tp": twin}, device_id_type=MESH,
        )

    def c_copy(which, o, sbuf, cbuf):
        return pltpu.make_async_remote_copy(
            src_ref=sbuf.at[o - 1], dst_ref=cbuf.at[o - 1],
            send_sem=c_send.at[which, o - 1], recv_sem=c_recv.at[which, o - 1],
            device_id={"tp": at_chip(o)}, device_id_type=MESH,
        )

    def rs_first(which, partial, pbuf, rbuf):
        for o in order:
            td = lax.rem(x + o, nx) * 2 + 1 - core
            pbuf[o] = partial(td).astype(BF)
            d_copy(which, o, pbuf, rbuf).start()

    def rs_second(which, partial, pbuf, rbuf, sbuf, cbuf):
        for o in order:
            mine = partial(at_chip(o))
            d_copy(which, o, pbuf, rbuf).wait_recv()
            both = mine + rbuf[o].astype(F32)
            if o:
                sbuf[o - 1] = both.astype(BF)
                c_copy(which, o, sbuf, cbuf).start()
            else:
                acc[...] = both

    def rs_third(which, sbuf, cbuf):
        total = acc[...]
        for o in order[:3]:
            c_copy(which, o, sbuf, cbuf).wait_recv()
            total = total + cbuf[o - 1].astype(F32)
        return total

    def rs_drain(which, pbuf, rbuf, sbuf, cbuf):
        for o in order:
            d_copy(which, o, pbuf, rbuf).wait_send()
            if o:
                c_copy(which, o, sbuf, cbuf).wait_send()

    def out_rows(td):
        return pl.ds(pl.multiple_of(td * rows, rows), rows)

    first(glus)
    for i, w in enumerate((wg, wu)):
        tail[i, own, :] = jnp.concatenate([w[:, main:], wd[:, main:]], axis=1)

    for c in locals_[3:]:
        c.wait()
    first(ms)
    first(ds)
    ag1[t] = stream[...].T
    ag_start(ag1, 0)
    units(1, 5)
    ag_forward(ag1, 0, (1, 3))
    unit(5)
    ag_forward(ag1, 0, (2,))
    unit(6)
    ag_finish(ag1, 0)
    normalize(ag1, mixer_gain, 0)
    unit(7)
    normalize(ag1, mixer_gain, 1)
    unit(8)
    normalize(ag1, mixer_gain, 2)
    pad[0:32, :] = jnp.zeros((32, chans), F32)
    units(9, 15)
    unit(15)
    unit(16)

    lanes = pl.ds(pl.multiple_of(t * chans, chans), chans)
    nb = 6
    bt = toks // nb

    def st_copy(o, src, target):
        return pltpu.make_async_remote_copy(
            src_ref=stats.at[src], dst_ref=stats.at[src],
            send_sem=st_send.at[o], recv_sem=st_recv.at[src],
            device_id={"tp": target}, device_id_type=MESH,
        )

    def gated():
        both = dot_nn(nrm[...], glu[:, 0:2 * chans])
        value = both[:, :chans] * jax.nn.sigmoid(both[:, chans:])
        pad[32:32 + toks, :] = value.astype(BF).astype(F32)

    def convolve(blocks):
        kern = conv_kernel[:, lanes].astype(F32)
        for b in blocks:
            total = jnp.zeros((bt, chans), F32)
            for k in range(taps):
                lo = b * bt + 32 - (taps - 1) + k
                total = total + kern[k:k + 1, :] * pad[lo:lo + bt, :]
            cvt[b * bt:(b + 1) * bt, :] = total

    def send_stats():
        flipped = cvt[...].T
        stats[t, 0:1, :] = jnp.sum(flipped, axis=0, keepdims=True)
        stats[t, 1:2, :] = jnp.sum(flipped * flipped, axis=0, keepdims=True)
        for o in range(1, nt):
            st_copy(o, t, lax.rem(t + o, nt)).start()

    def mixed_part(td):
        return dot_nt(glu[out_rows(td), 2 * chans:3 * chans], act[...])

    def activate():
        for o in range(1, nt):
            st_copy(o, lax.rem(t + o, nt), lax.rem(t + o, nt)).wait_recv()
        total = stats[0]
        for j in range(1, nt):
            total = total + stats[j]
        total = total / (chans * nt)
        mean, msq = total[0:1], total[1:2]
        inv = lax.rsqrt(msq - mean * mean + 1e-05)
        cols = jnp.concatenate([mean, inv, jnp.zeros((6, toks), F32)], axis=0).T
        scaled = (cvt[...] - cols[:, 0:1]) * cols[:, 1:2] * channel_gain[:, lanes]
        act[...] = (scaled * jax.nn.sigmoid(scaled)).astype(BF)

    def middle():
        mid[...] = (stream[...].astype(F32) + rs_third(0, sb, cb)).astype(BF)
        ag2[t] = mid[...].T
        ag_start(ag2, 1)

    def hand_over():
        for d, n in ((CW, ncw), (CCW, nccw)):
            @pl.loop(1, n + 1)
            def _(s):
                ycopy(d, s, 1 - gi).wait_recv()
                ytcopy(d, s, 1 - gi).wait_recv()

    def hide():
        rest = tail.shape[2] // 2
        for lo in range(0, main, 256):
            hi = min(lo + 256, main)
            gate = dot_nn(nrm[...], gu[0, :, lo:hi])
            up = dot_nn(nrm[...], gu[1, :, lo:hi])
            hid[:, lo:hi] = (gate * jax.nn.sigmoid(gate) * up).astype(BF)
        gate, up = dot_nn(nrm[...], tail[0]), dot_nn(nrm[...], tail[1])
        gate, up = gate[:, :rest], up[:, :rest]
        ends = gate * jax.nn.sigmoid(gate) * up
        hid[:, main:] = jnp.concatenate([jnp.zeros_like(ends), ends], axis=1).astype(BF)

    events = (
        gated,
        lambda: convolve(range(nb // 2)),
        lambda: [convolve(range(nb // 2, nb)), send_stats()],
        activate,
        lambda: rs_first(0, mixed_part, pb, rb),
        lambda: rs_second(0, mixed_part, pb, rb, sb, cb),
        middle,
        lambda: ag_forward(ag2, 1, (1, 3)),
        lambda: ag_forward(ag2, 1, (2,)),
        lambda: ag_finish(ag2, 1),
        lambda: [normalize(ag2, ffn_gain, b) for b in range(3)],
        hand_over,
        hide,
    )
    mid_step = ncw // 2 + 1
    rest_steps = [(ms, s) for s in range(mid_step, mid_step + LEAD)]
    for s in range(mid_step, ncw + 1):
        if s + LEAD <= ncw:
            rest_steps.append((ms, s + LEAD))
        rest_steps.append((ds, s))
    for k in range(2 * len(rest_steps) + 1):
        if k:
            pieces, s = rest_steps[(k - 1) // 2]
            any_step(s, pieces[:2] if k % 2 else pieces[2:])
        for at, event in zip(PLACES, events):
            if at == k:
                event()

    def ffn_part(td):
        r = out_rows(td)
        return dot_nt(dn[r, :], hid[:, :main]) + dot_nt(tail[0, r, :], hid[:, main:])

    rs_first(1, ffn_part, pb2, rb2)
    rs_second(1, ffn_part, pb2, rb2, sb2, cb2)

    for p in glus + ms + ds:
        for d in (CW, CCW):
            n = ncw if d == far_way(p) else nccw
            if p < 2:
                ref = glu.at[pl.ds(0, n * half), :]
            elif p < 6:
                ref = gu.at[0, pl.ds(0, n * quarter), :]
            elif p < 10:
                ref = dn.at[pl.ds(0, n * quarter), :]
            else:
                ref = tail.at[0, pl.ds(0, n * srows), :]
            pltpu.make_async_copy(ref, ref, zsend.at[d, p]).wait()
    ref = gu.at[0, pl.ds(0, (nz - 1) * srows), :]
    pltpu.make_async_copy(ref, ref, ysend).wait()
    ref = tail.at[0, pl.ds(0, (nz - 1) * srows), :]
    pltpu.make_async_copy(ref, ref, ytsend).wait()
    ag_drain(ag1, 0)
    ag_drain(ag2, 1)
    for o in range(1, nt):
        st_copy(o, t, twin).wait_send()
    rs_drain(0, pb, rb, sb, cb)

    out[...] = (mid[...].astype(F32) + rs_third(1, sb2, cb2)).astype(BF)
    rs_drain(1, pb2, rb2, sb2, cb2)


def solution(mesh):
    nz, nt = mesh.shape["fs"], mesh.shape["tp"]

    def on_device(
        stream, mixer_gain, glu_value, glu_gate, conv_kernel, channel_gain,
        conv_out, ffn_gain, ffn_gate, ffn_up, ffn_down,
    ):
        rows, toks = stream.shape
        srows, chans = glu_value.shape
        ff = ffn_gate.shape[1]
        main = ff // 128 * 128
        width = rows * nt
        nx = nt // 2
        vm = pl.BlockSpec(memory_space=pltpu.VMEM)
        hbm = pl.BlockSpec(memory_space=pl.ANY)
        dma = pltpu.SemaphoreType.DMA
        blocks = [
            pltpu.VMEM((nx, rows, toks), BF),
            pltpu.VMEM((nx, rows, toks), BF),
            pltpu.VMEM((nx - 1, rows, toks), BF),
            pltpu.VMEM((nx - 1, rows, toks), BF),
        ]
        return pl.pallas_call(
            functools.partial(kernel, nz, nt),
            out_shape=jax.ShapeDtypeStruct((rows, toks), BF),
            in_specs=[vm] * 5 + [hbm] * 3 + [vm] * 3,
            out_specs=vm,
            scratch_shapes=[
                pltpu.VMEM((width, 3 * chans), BF),
                pltpu.VMEM((2, width, main), BF),
                pltpu.VMEM((width, main), BF),
                pltpu.VMEM((2, width, 2 * (ff - main)), BF),
                pltpu.VMEM((nt, toks, rows), BF),
                pltpu.VMEM((nt, toks, rows), BF),
                pltpu.VMEM((toks, width), BF),
                pltpu.VMEM((toks + 32, chans), F32),
                pltpu.VMEM((toks, chans), F32),
                pltpu.VMEM((toks, chans), BF),
                pltpu.VMEM((nt, 2, toks), F32),
                pltpu.VMEM((toks, main + 2 * (ff - main)), BF),
                pltpu.VMEM((rows, toks), F32),
                pltpu.VMEM((rows, toks), BF),
                *blocks, *blocks,
                dma((6,)),
                dma((2, 11)),
                dma((2, 11, nz // 2)),
                dma,
                dma((nz,)),
                dma,
                dma((nz,)),
                dma((2, 4 + nx - 1)),
                dma((2, nt)),
                dma((nt,)),
                dma((nt,)),
                dma((2, nx)),
                dma((2, nx)),
                dma((2, nx - 1)),
                dma((2, nx - 1)),
            ],
            compiler_params=pltpu.CompilerParams(collective_id=0, has_side_effects=True),
        )(
            stream, mixer_gain[None, :], conv_kernel, channel_gain[None, :],
            ffn_gain[None, :], glu_value, glu_gate, conv_out, ffn_gate, ffn_up, ffn_down,
        )

    weight = P("fs", "tp")
    in_specs = (
        P("tp", ("grp", "fs")), P(), weight, weight, P(), P(), weight, P(),
        weight, weight, weight,
    )
    return jax.shard_map(
        on_device, mesh=mesh, in_specs=in_specs,
        out_specs=P("tp", ("grp", "fs")), check_vma=False,
    )
```
